1024 devices in a mesh: gr: 2 (over z_hi), sp: 64 (over z_lo, y), tp: 8 (over x, core).
Axes of the slice: x: 4, y: 8, z: 16 (z_hi: 2, z_lo: 8; z = z_hi * 8 + z_lo), core: 2. Of those that a mesh axis runs over, the one named last changes fastest.
Arguments:
- tokens: bfloat16 [64, 8192, 2048], P(('gr', 'tp'), 'sp'), may hold values from -6 to 6
- kv_weight: bfloat16 [2048, 1024], replicated, may hold values from -0.125 to 0.125
- queries: bfloat16 [64, 1536], P(('gr', 'tp')), may hold values from -6 to 6
- score_offset: float32 [24], replicated, may hold values from -10.5 to -3.5
Outputs:
- cache: bfloat16 [16, 64, 8192, 64], P(('gr', 'tp'), 'sp')
- read: bfloat16 [64, 1536], P(('gr', 'tp'))
The draws below stay inside these ranges and needn't reach their ends.
All inputs are finite; a program needn't handle non-finite values.
Results may differ from the reference program's by a relative error of at most 0.0085.
Values may be sent and summed in bfloat16 or wider, within the bound.
No kernel may reach another device: no remote copies, remote signals or barrier semaphores. Data moves between devices by JAX's collectives and lax.ppermute only.
A program may use at most 32 MiB of HBM per device.

```python
import jax
import jax.numpy as jnp
from jax import lax

D = 2048
H = 24
KVH = 8
HD = 64
LEN = 8192
KVF = 1024
CB = 16
W = 64
SEQ_DEV = 4
GROUPS = 16
SEQS = 64
N_SP = 64


def levels(own_key, dims, pieces, low, top_value):
    def one(dim, parts):
        draws = jax.random.uniform(jax.random.fold_in(jax.random.fold_in(own_key, 6), dim), (parts,), jnp.float32, low / len(pieces), top_value / len(pieces))
        return jnp.repeat(jnp.exp(draws), dims[dim] // parts).reshape((-1,) + (1,) * (len(dims) - dim - 1))

    loudness = one(*pieces[0])
    for cut in pieces[1:]:
        loudness = loudness * one(*cut)
    return loudness


def bell_draw(own_key, dims, scale, reach, pieces=(), dtype=jnp.bfloat16):
    entries = scale * jax.random.normal(own_key, dims, jnp.float32)
    if pieces:
        entries = entries * levels(own_key, dims, pieces, -0.22, 0.18)
    return jnp.clip(entries, -reach, reach).astype(dtype)


def setup_inputs(seed: int = 0) -> dict:
    key_list = jax.random.split(jax.random.key(seed), 5)
    tokens = bell_draw(key_list[0], (SEQS, LEN, D), 1.0, 6.0, ((0, 16), (1, 64)))
    kv_weight = bell_draw(key_list[1], (D, KVF), D ** -0.5, 0.125)
    queries = bell_draw(key_list[2], (SEQS, H * HD), 1.0, 6.0, ((0, 16),))
    score_offset = jnp.clip(jax.random.uniform(key_list[3], (H,), jnp.float32, -10.5, -3.5), -10.5, -3.5)
    return dict(tokens=tokens, kv_weight=kv_weight, queries=queries, score_offset=score_offset)


def reference(tokens, kv_weight, queries, score_offset):
    projected = jnp.dot(tokens.reshape(SEQS * LEN, D), kv_weight, preferred_element_type=jnp.float32).astype(jnp.bfloat16)
    projected = projected.reshape(SEQS, LEN, KVF)
    cache = projected.reshape(GROUPS, SEQ_DEV, LEN, CB, W).transpose(0, 1, 3, 2, 4).reshape(GROUPS, N_SP, LEN, W)
    pairs = projected.reshape(SEQS, LEN, 2, KVH, HD)
    offsets = score_offset.reshape(KVH, H // KVH)

    def one_sequence(args):
        query_row, pair_rows = args
        query_heads = query_row.astype(jnp.float32).reshape(KVH, H // KVH, HD)
        key_rows = pair_rows[:, 0].astype(jnp.float32)
        value_rows = pair_rows[:, 1].astype(jnp.float32)
        logits = jnp.einsum('ngd,pnd->ngp', query_heads, key_rows) * (HD ** -0.5) + offsets[:, :, None]
        keep_log = jax.nn.log_sigmoid(-logits)
        between = lax.cumsum(keep_log, axis=2, reverse=True) - keep_log
        weights = jnp.exp(jax.nn.log_sigmoid(logits) + between)
        return jnp.einsum('ngp,pnd->ngd', weights, value_rows).reshape(H * HD)

    read = lax.map(one_sequence, (queries, pairs)).astype(jnp.bfloat16)
    return cache, read
```

```python
import functools

import jax
import jax.numpy as jnp
from jax import lax
from jax.experimental import pallas as pl
from jax.experimental.pallas import tpu as pltpu
from jax.sharding import Mesh
from jax.sharding import PartitionSpec as P


KVH = 8
HD = 64
LANES = 128
SLOT = 32
SP = ("sp_0", "sp_1")
VMEM = pltpu.VMEM


def small(mebibytes):
    return pltpu.CompilerParams(vmem_limit_bytes=mebibytes * 1024 * 1024)


def project_kernel(x_ref, w_ref, out_ref):
    seqs, rows, depth = x_ref.shape
    acc = jnp.dot(
        x_ref[...].reshape(seqs * rows, depth), w_ref[...], preferred_element_type=jnp.float32
    )
    for q in range(seqs):
        turned = acc[q * rows : (q + 1) * rows].T
        out_ref[q] = turned.reshape(out_ref.shape[1:]).astype(out_ref.dtype)


def project(tokens, kv_weight, blocks):
    seqs, rows, depth = tokens.shape
    features = kv_weight.shape[1]
    width = features // blocks
    step = 256
    return pl.pallas_call(
        project_kernel,
        grid=(features // step,),
        in_specs=[
            pl.BlockSpec((seqs, rows, depth), lambda j: (0, 0, 0)),
            pl.BlockSpec((depth, step), lambda j: (0, j)),
        ],
        out_specs=pl.BlockSpec((seqs, step // width, width, rows), lambda j: (0, j, 0, 0)),
        out_shape=jax.ShapeDtypeStruct((seqs, blocks, width, rows), jnp.bfloat16),
        name="project",
    )(tokens, kv_weight)


def stick_kernel(heads, kv_ref, q_ref, off_ref, out_ref):
    seqs = kv_ref.shape[0]
    group = heads // KVH
    f32 = jnp.float32
    row_head = lax.broadcasted_iota(jnp.int32, (SLOT, LANES), 0) // group
    logits = []
    for s in range(seqs):
        queries = q_ref[s * SLOT : (s + 1) * SLOT]
        total = jnp.zeros((SLOT, LANES), f32)
        for n in range(KVH):
            part = jnp.dot(queries, kv_ref[s, n], preferred_element_type=f32)
            total = jnp.where(row_head == n, part, total)
        logits.append(total)
    logit = jnp.concatenate(logits, axis=0) * HD ** (-0.5) + off_ref[...]
    soft = jnp.log1p(jnp.exp(-jnp.abs(logit)))
    log_take = jnp.minimum(logit, 0.0) - soft
    keep = jnp.minimum(-logit, 0.0) - soft
    r = lax.broadcasted_iota(jnp.int32, (LANES, LANES), 0)
    c = lax.broadcasted_iota(jnp.int32, (LANES, LANES), 1)
    later = (r > c).astype(f32)
    between = jnp.dot(keep, later, preferred_element_type=f32, precision=lax.Precision.HIGHEST)
    weight = jnp.exp(log_take + between)
    high = weight.astype(jnp.bfloat16)
    low = (weight - high.astype(f32)).astype(jnp.bfloat16)
    lane = lax.broadcasted_iota(jnp.int32, (HD, LANES), 1)
    lane_seq, lane_head = lane // SLOT, (lane % SLOT) // group
    dims = (((1,), (1,)), ((), ()))
    total = jnp.zeros((HD, LANES), f32)
    for s in range(seqs):
        values = kv_ref[s, KVH:].reshape(KVH * HD, LANES)
        product = lax.dot_general(values, high, dims, preferred_element_type=f32)
        product += lax.dot_general(values, low, dims, preferred_element_type=f32)
        for n in range(KVH):
            mine = (lane_seq == s) & (lane_head == n)
            total = jnp.where(mine, product[n * HD : (n + 1) * HD], total)
    out_ref[:HD] = total
    out_ref[HD:] = lax.dot_general(
        jnp.ones((8, LANES), f32), keep, dims, preferred_element_type=f32,
        precision=lax.Precision.HIGHEST,
    )


def stick(projected, queries, score_offset):
    seqs = queries.shape[0]
    heads = score_offset.shape[0]
    spare = SLOT - heads
    rows = jnp.pad(queries.reshape(seqs, heads, HD), ((0, 0), (0, spare), (0, 0)))
    offsets = jnp.tile(jnp.pad(score_offset, (0, spare)), seqs)[:, None]
    return pl.pallas_call(
        functools.partial(stick_kernel, heads),
        in_specs=[pl.BlockSpec(memory_space=VMEM)] * 3,
        out_specs=pl.BlockSpec(memory_space=VMEM),
        out_shape=jax.ShapeDtypeStruct((HD + 8, LANES), jnp.float32),
        compiler_params=small(4),
        name="stick",
    )(projected, rows.reshape(seqs * SLOT, HD), offsets)


def partner(block, axis, distance):
    return lax.ppermute(block, axis, [(i, i ^ distance) for i in range(lax.axis_size(axis))])


def pack(state):
    total = state[HD:]
    high = total.astype(jnp.bfloat16).astype(jnp.float32)
    middle = (total - high).astype(jnp.bfloat16).astype(jnp.float32)
    row = lax.broadcasted_iota(jnp.int32, total.shape, 0)
    parts = jnp.where(row == 0, high, jnp.where(row == 1, middle, total - high - middle))
    return jnp.concatenate([state[:HD], parts], axis=0).astype(jnp.bfloat16)


def join_kernel(axis, distance, own_ref, other_ref, out_ref):
    own_first = (lax.axis_index(axis) & distance) == 0
    own, other = own_ref[...], other_ref[...]
    first = jnp.where(own_first, own, other)
    last = jnp.where(own_first, other, own)
    values = first[:HD] * jnp.exp(last[HD : HD + 1]) + last[:HD]
    state = jnp.concatenate([values, first[HD:] + last[HD:]], axis=0)
    out_ref[...] = pack(state) if out_ref.dtype == jnp.bfloat16 else state


def join(own, other, axis, distance, dtype):
    return pl.pallas_call(
        functools.partial(join_kernel, axis, distance),
        in_specs=[pl.BlockSpec(memory_space=VMEM)] * 2,
        out_specs=pl.BlockSpec(memory_space=VMEM),
        out_shape=jax.ShapeDtypeStruct(own.shape, dtype),
        compiler_params=small(1),
        name="join",
    )(own, other)


def finish_kernel(heads, own_ref, other_ref, out_ref, turned, wide):
    seqs = out_ref.shape[0]
    place = lax.axis_index("sp_0")
    total = jnp.zeros((HD, LANES), jnp.float32)
    after = jnp.zeros((1, LANES), jnp.float32)
    half = own_ref.shape[0]
    for z in reversed(range(2 * half)):
        at = place ^ z
        state = jnp.where(at % 2 == 0, own_ref[at // 2].astype(jnp.float32), other_ref[at // 2].astype(jnp.float32))
        total += state[:HD] * jnp.exp(after)
        after += state[HD : HD + 1] + state[HD + 1 : HD + 2] + state[HD + 2 : HD + 3]
    turned[...] = jnp.concatenate([total, total], axis=0).T
    for h in range(heads):
        wide[:, h * HD : (h + 1) * HD] = turned[pl.ds(h, seqs, stride=SLOT), :][:, :HD]
    out_ref[...] = wide[...].astype(out_ref.dtype)


def finish(own, other, seqs, heads):
    return pl.pallas_call(
        functools.partial(finish_kernel, heads),
        in_specs=[pl.BlockSpec(memory_space=VMEM)] * 2,
        out_specs=pl.BlockSpec(memory_space=VMEM),
        out_shape=jax.ShapeDtypeStruct((seqs, heads * HD), jnp.bfloat16),
        scratch_shapes=[
            pltpu.VMEM((LANES, LANES), jnp.float32),
            pltpu.VMEM((seqs, heads * HD), jnp.float32),
        ],
        compiler_params=small(1),
        name="finish",
    )(own, other)


def lay_kernel(in_ref, out_ref, sem):
    sources, _, rows = in_ref.shape
    for i in range(sources):
        pltpu.make_async_copy(in_ref.at[i], out_ref.at[:, pl.ds(i * rows, rows)], sem).start()
    pltpu.make_async_copy(out_ref, out_ref, sem).wait()


def lay(received):
    sources, width, rows = received.shape
    return pl.pallas_call(
        lay_kernel,
        in_specs=[pl.BlockSpec(memory_space=pl.ANY)],
        out_specs=pl.BlockSpec(memory_space=pl.ANY),
        out_shape=jax.ShapeDtypeStruct((width, sources * rows), received.dtype),
        scratch_shapes=[pltpu.SemaphoreType.DMA],
        compiler_params=small(1),
        name="lay",
    )(received)


def local(tokens, kv_weight, queries, score_offset):
    seqs, rows, _ = tokens.shape
    features = kv_weight.shape[1]
    slots = lax.axis_size(SP)
    blocks = slots // seqs
    width = features // blocks
    heads = score_offset.shape[0]

    projected = project(tokens, kv_weight, blocks)
    received = lax.all_to_all(
        projected.reshape(slots, width, rows), SP, split_axis=0, concat_axis=0, tiled=True
    )
    laid = lay(received)
    cache = laid.T.reshape(1, 1, slots * rows, width)

    state = stick(projected, queries, score_offset)
    for distance in (1, 2, 4):
        dtype = jnp.bfloat16 if distance == 4 else jnp.float32
        state = join(state, partner(state, "sp_1", distance), "sp_1", distance, dtype)
    own = jnp.stack([state] + [partner(state, "sp_0", d) for d in (2, 4, 6)])
    other = partner(own, "sp_0", 1)
    read = finish(own, other, seqs, heads)
    return cache, read


def solution(mesh):
    torus = Mesh(
        mesh.devices.reshape(mesh.shape["gr"], 8, 8, mesh.shape["tp"]), ("gr", "sp_0", "sp_1", "tp")
    )
    return jax.shard_map(
        local,
        mesh=torus,
        in_specs=(P(("gr", "tp"), SP, None), P(), P(("gr", "tp"), None), P()),
        out_specs=(P(("gr", "tp"), SP, None, None), P(("gr", "tp"), None)),
        check_vma=False,
    )
```

```python
import functools

import jax
import jax.numpy as jnp
from jax import lax
from jax.experimental import pallas as pl
from jax.experimental.pallas import tpu as pltpu
from jax.sharding import Mesh
from jax.sharding import PartitionSpec as P


KVH = 8
HD = 64
LANES = 128
SLOT = 32
ROWS = HD + 8
DEPTH = 256
SP = ("sp_0", "sp_1")
VMEM = pltpu.VMEM
BF16 = jnp.bfloat16
F32 = jnp.float32
BY_POSITION = (((1,), (1,)), ((), ()))


def pack(values, total):
    high = total.astype(BF16).astype(F32)
    middle = (total - high).astype(BF16).astype(F32)
    row = lax.broadcasted_iota(jnp.int32, total.shape, 0)
    parts = jnp.where(row == 0, high, jnp.where(row == 1, middle, total - high - middle))
    return jnp.concatenate([values, parts], axis=0).astype(BF16)


def unpack(state):
    state = state.astype(F32)
    return state[:HD], state[HD : HD + 1] + state[HD + 1 : HD + 2] + state[HD + 2 : HD + 3]


def fold(first, last):
    return first[0] * jnp.exp(last[1]) + last[0], first[1] + last[1]


def choose(condition, one, other):
    return tuple(jnp.where(condition, a, b) for a, b in zip(one, other))


def head_rows(query_ref, offset_ref, rows):
    seqs = query_ref.shape[0]
    heads = offset_ref.shape[0]
    rows[...] = jnp.zeros_like(rows)
    row = lax.broadcasted_iota(jnp.int32, (SLOT, LANES), 0)
    offset = jnp.zeros((SLOT, LANES), F32)
    for h in range(heads):
        rows[pl.ds(h, seqs, stride=SLOT), :HD] = query_ref[:, h * HD : (h + 1) * HD].astype(F32)
        offset = jnp.where(row == h, offset_ref[h], offset)
    return offset


def split(x, parts):
    pieces = []
    for _ in range(parts):
        piece = x.astype(BF16)
        pieces.append(piece)
        x = x - piece.astype(F32)
    return jnp.concatenate(pieces, axis=0)


def stick(kv, rows, offset, group):
    seqs = kv.shape[0]
    slots = seqs * SLOT
    row_head = lax.broadcasted_iota(jnp.int32, (SLOT, LANES), 0) // group
    logits = []
    for s in range(seqs):
        queries = rows[s * SLOT : (s + 1) * SLOT, :HD].astype(BF16)
        total = jnp.zeros((SLOT, LANES), F32)
        for n in range(KVH):
            part = jnp.dot(queries, kv[s, n], preferred_element_type=F32)
            total = jnp.where(row_head == n, part, total)
        logits.append(total * HD ** (-0.5) + offset)
    logit = jnp.concatenate(logits, axis=0)
    soft = jnp.log1p(jnp.exp(-jnp.abs(logit)))
    log_take = jnp.minimum(logit, 0.0) - soft
    keep = jnp.minimum(-logit, 0.0) - soft
    r = lax.broadcasted_iota(jnp.int32, (LANES, LANES), 0)
    c = lax.broadcasted_iota(jnp.int32, (LANES, LANES), 1)
    sums = jnp.dot(split(keep, 3), (r > c).astype(BF16), preferred_element_type=F32)
    between = sums[:slots] + sums[slots : 2 * slots] + sums[2 * slots :]
    weight = jnp.exp(log_take + between)
    read = []
    for s in range(seqs):
        weights = split(weight[s * SLOT : (s + 1) * SLOT], 2)
        values = kv[s, KVH:].reshape(KVH * HD, LANES)
        product = lax.dot_general(weights, values, BY_POSITION, preferred_element_type=F32)
        product = product[:SLOT] + product[SLOT:]
        halves = [jnp.zeros((SLOT, LANES), F32), jnp.zeros((SLOT, LANES), F32)]
        for n in range(KVH):
            piece = product[:, n // 2 * LANES : (n // 2 + 1) * LANES]
            halves[n % 2] = jnp.where(row_head == n, piece, halves[n % 2])
        read.append(jnp.where(row_head % 2 == 0, halves[0], pltpu.roll(halves[1], HD, 1)))
    total = (between + keep)[:, :1]
    state = jnp.where(c < HD, jnp.concatenate(read, axis=0), total).T
    return pack(state[:HD], state[HD:ROWS])


def project_kernel(
    x_hbm, w_hbm, query_ref, offset_ref, out_hbm, state_ref, x, w, out, rows, x_sem, w_sem, out_sem
):
    seqs, positions, depth = x.shape
    steps = depth // DEPTH
    parts = [pl.ds(i * DEPTH, DEPTH) for i in range(steps)]
    x_in = [pltpu.make_async_copy(x_hbm.at[:, :, p], x.at[:, :, p], x_sem.at[i]) for i, p in enumerate(parts)]
    w_in = [pltpu.make_async_copy(w_hbm.at[p], w.at[p], w_sem.at[i]) for i, p in enumerate(parts)]
    for i in range(steps):
        x_in[i].start()
        w_in[i].start()
    offset = head_rows(query_ref, offset_ref, rows)
    acc = None
    for i in range(steps):
        x_in[i].wait()
        w_in[i].wait()
        part = jnp.dot(
            x[:, :, i * DEPTH : (i + 1) * DEPTH].reshape(seqs * positions, DEPTH),
            w[i * DEPTH : (i + 1) * DEPTH],
            preferred_element_type=F32,
        )
        acc = part if acc is None else acc + part
    copies = []
    for s in range(seqs):
        turned = acc[s * positions : (s + 1) * positions].T
        out[s] = turned.reshape(out.shape[1:]).astype(BF16)
        copies.append(pltpu.make_async_copy(out.at[s], out_hbm.at[s], out_sem.at[s]))
        copies[-1].start()
    state_ref[...] = stick(out, rows, offset, offset_ref.shape[0] // KVH)
    for copy in copies:
        copy.wait()


def project(tokens, kv_weight, queries, score_offset, blocks):
    seqs, positions, depth = tokens.shape
    features = kv_weight.shape[1]
    shape = (seqs, blocks, features // blocks, positions)
    dma = pltpu.SemaphoreType.DMA
    return pl.pallas_call(
        project_kernel,
        in_specs=[
            pl.BlockSpec(memory_space=pl.ANY),
            pl.BlockSpec(memory_space=pl.ANY),
            pl.BlockSpec(memory_space=VMEM),
            pl.BlockSpec(memory_space=pltpu.SMEM),
        ],
        out_specs=[pl.BlockSpec(memory_space=pl.ANY), pl.BlockSpec(memory_space=VMEM)],
        out_shape=[jax.ShapeDtypeStruct(shape, BF16), jax.ShapeDtypeStruct((ROWS, LANES), BF16)],
        scratch_shapes=[
            VMEM(tokens.shape, BF16),
            VMEM(kv_weight.shape, BF16),
            VMEM(shape, BF16),
            VMEM((seqs * SLOT, LANES), F32),
            dma((depth // DEPTH,)),
            dma((depth // DEPTH,)),
            dma((seqs,)),
        ],
        name="project",
    )(tokens, kv_weight, queries, score_offset)


def partner(block, axis, distance):
    return lax.ppermute(block, axis, [(i, i ^ distance) for i in range(lax.axis_size(axis))])


def small(mebibytes):
    return pltpu.CompilerParams(vmem_limit_bytes=mebibytes * 1024 * 1024)


def merge(place, states):
    run = None
    for at in reversed(range(len(states))):
        state = states[0]
        for i in range(1, len(states)):
            state = choose((place ^ at) == i, states[i], state)
        run = state if run is None else fold(state, run)
    return run


def join_kernel(shift, *refs):
    state_refs, out_ref = refs[:-1], refs[-1]
    place = (lax.axis_index("sp_1") >> shift) % len(state_refs)
    for i in range(out_ref.shape[0]):
        values, total = merge(place, [unpack(ref[i]) for ref in state_refs])
        out_ref[i] = pack(values, jnp.broadcast_to(total, (8, LANES)))


def join(runs, shift):
    return pl.pallas_call(
        functools.partial(join_kernel, shift),
        in_specs=[pl.BlockSpec(memory_space=VMEM)] * len(runs),
        out_specs=pl.BlockSpec(memory_space=VMEM),
        out_shape=jax.ShapeDtypeStruct(runs[0].shape, BF16),
        compiler_params=small(2),
        name="join",
    )(*runs)


def finish_kernel(heads, *refs):
    state_refs, (out_ref, turned, wide) = refs[:-3], refs[-3:]
    seqs = out_ref.shape[0]
    states = [unpack(ref[i]) for i in range(2) for ref in state_refs]
    values, _ = merge(lax.axis_index("sp_0"), states)
    turned[...] = jnp.concatenate([values, values], axis=0).T
    for h in range(heads):
        wide[:, h * HD : (h + 1) * HD] = turned[pl.ds(h, seqs, stride=SLOT), :][:, :HD]
    out_ref[...] = wide[...].astype(out_ref.dtype)


def finish(runs, seqs, heads):
    return pl.pallas_call(
        functools.partial(finish_kernel, heads),
        in_specs=[pl.BlockSpec(memory_space=VMEM)] * len(runs),
        out_specs=pl.BlockSpec(memory_space=VMEM),
        out_shape=jax.ShapeDtypeStruct((seqs, heads * HD), BF16),
        scratch_shapes=[VMEM((LANES, LANES), F32), VMEM((seqs, heads * HD), F32)],
        compiler_params=small(2),
        name="finish",
    )(*runs)


def lay_kernel(in_ref, out_ref, sem):
    sources, _, positions = in_ref.shape
    for i in range(sources):
        place = pl.ds(i * positions, positions)
        pltpu.make_async_copy(in_ref.at[i], out_ref.at[:, place], sem).start()
    pltpu.make_async_copy(out_ref, out_ref, sem).wait()


def lay(received):
    sources, width, positions = received.shape
    return pl.pallas_call(
        lay_kernel,
        in_specs=[pl.BlockSpec(memory_space=pl.ANY)],
        out_specs=pl.BlockSpec(memory_space=pl.ANY),
        out_shape=jax.ShapeDtypeStruct((width, sources * positions), received.dtype),
        scratch_shapes=[pltpu.SemaphoreType.DMA],
        compiler_params=small(1),
        name="lay",
    )(received)


def local(tokens, kv_weight, queries, score_offset):
    seqs, positions, _ = tokens.shape
    features = kv_weight.shape[1]
    slots = lax.axis_size(SP)
    blocks = slots // seqs
    width = features // blocks
    heads = score_offset.shape[0]

    projected, state = project(tokens, kv_weight, queries, score_offset, blocks)
    opposite = partner(state, "sp_0", 4)
    received = lax.all_to_all(
        projected.reshape(slots, width, positions), SP, split_axis=0, concat_axis=0, tiled=True
    )
    laid = lay(received)
    cache = laid.T.reshape(1, 1, slots * positions, width)

    runs = jnp.stack([state, opposite])
    runs = join([runs] + [partner(runs, "sp_1", d) for d in (1, 2, 3)], 0)
    runs = join([runs, partner(runs, "sp_1", 4)], 2)
    gathered = [runs]
    for distance in (1, 2, 3):
        gathered.append(partner(runs, "sp_0", distance))
    read = finish(gathered, seqs, heads)
    return cache, read


def solution(mesh):
    torus = Mesh(
        mesh.devices.reshape(mesh.shape["gr"], 8, 8, mesh.shape["tp"]), ("gr", "sp_0", "sp_1", "tp")
    )
    return jax.shard_map(
        local,
        mesh=torus,
        in_specs=(P(("gr", "tp"), SP, None), P(), P(("gr", "tp"), None), P()),
        out_specs=(P(("gr", "tp"), SP, None, None), P(("gr", "tp"), None)),
        check_vma=False,
    )
```

```python
import functools

import jax
import jax.numpy as jnp
from jax import lax
from jax.experimental import pallas as pl
from jax.experimental.pallas import tpu as pltpu
from jax.sharding import Mesh
from jax.sharding import PartitionSpec as P


KVH = 8
HD = 64
LANES = 128
SLOT = 32
SIDE = 8
ROWS = HD + 8
DEPTH = 256
SP = ("sp_0", "sp_1")
VMEM = pltpu.VMEM
BF16 = jnp.bfloat16
F32 = jnp.float32
BY_POSITION = (((1,), (1,)), ((), ()))


def pack(values, total):
    high = total.astype(BF16).astype(F32)
    middle = (total - high).astype(BF16).astype(F32)
    row = lax.broadcasted_iota(jnp.int32, total.shape, 0)
    parts = jnp.where(row == 0, high, jnp.where(row == 1, middle, total - high - middle))
    return jnp.concatenate([values, parts], axis=0).astype(BF16)


def unpack(state):
    state = state.astype(F32)
    return state[:HD], state[HD : HD + 1] + state[HD + 1 : HD + 2] + state[HD + 2 : HD + 3]


def fold(first, last):
    return first[0] * jnp.exp(last[1]) + last[0], first[1] + last[1]


def choose(condition, one, other):
    return tuple(jnp.where(condition, a, b) for a, b in zip(one, other))


def head_rows(query_ref, offset_ref, rows):
    seqs = query_ref.shape[0]
    heads = offset_ref.shape[0]
    rows[...] = jnp.zeros_like(rows)
    row = lax.broadcasted_iota(jnp.int32, (SLOT, LANES), 0)
    offset = jnp.zeros((SLOT, LANES), F32)
    for h in range(heads):
        rows[pl.ds(h, seqs, stride=SLOT), :HD] = query_ref[:, h * HD : (h + 1) * HD].astype(F32)
        offset = jnp.where(row == h, offset_ref[h], offset)
    return offset


def split(x, parts):
    pieces = []
    for _ in range(parts):
        piece = x.astype(BF16)
        pieces.append(piece)
        x = x - piece.astype(F32)
    return jnp.concatenate(pieces, axis=0)


def stick(kv, rows, offset, group):
    seqs = kv.shape[0]
    slots = seqs * SLOT
    row_head = lax.broadcasted_iota(jnp.int32, (SLOT, LANES), 0) // group
    logits = []
    for s in range(seqs):
        queries = rows[s * SLOT : (s + 1) * SLOT, :HD].astype(BF16)
        total = jnp.zeros((SLOT, LANES), F32)
        for n in range(KVH):
            part = jnp.dot(queries, kv[s, n], preferred_element_type=F32)
            total = jnp.where(row_head == n, part, total)
        logits.append(total * HD ** (-0.5) + offset)
    logit = jnp.concatenate(logits, axis=0)
    soft = jnp.log1p(jnp.exp(-jnp.abs(logit)))
    log_take = jnp.minimum(logit, 0.0) - soft
    keep = jnp.minimum(-logit, 0.0) - soft
    r = lax.broadcasted_iota(jnp.int32, (LANES, LANES), 0)
    c = lax.broadcasted_iota(jnp.int32, (LANES, LANES), 1)
    sums = jnp.dot(split(keep, 3), (r > c).astype(BF16), preferred_element_type=F32)
    between = sums[:slots] + sums[slots : 2 * slots] + sums[2 * slots :]
    weight = jnp.exp(log_take + between)
    read = []
    for s in range(seqs):
        weights = split(weight[s * SLOT : (s + 1) * SLOT], 2)
        values = kv[s, KVH:].reshape(KVH * HD, LANES)
        product = lax.dot_general(weights, values, BY_POSITION, preferred_element_type=F32)
        product = product[:SLOT] + product[SLOT:]
        halves = [jnp.zeros((SLOT, LANES), F32), jnp.zeros((SLOT, LANES), F32)]
        for n in range(KVH):
            piece = product[:, n // 2 * LANES : (n // 2 + 1) * LANES]
            halves[n % 2] = jnp.where(row_head == n, piece, halves[n % 2])
        read.append(jnp.where(row_head % 2 == 0, halves[0], pltpu.roll(halves[1], HD, 1)))
    total = (between + keep)[:, :1]
    state = jnp.where(c < HD, jnp.concatenate(read, axis=0), total).T
    return pack(state[:HD], state[HD:ROWS])


def project_kernel(
    x_hbm,
    w_hbm,
    query_ref,
    offset_ref,
    out_hbm,
    keep_ref,
    send_ref,
    x,
    w,
    out,
    rows,
    x_sem,
    w_sem,
    out_sem,
):
    seqs, positions, depth = x.shape
    steps = depth // DEPTH
    parts = [pl.ds(i * DEPTH, DEPTH) for i in range(steps)]
    x_in = [pltpu.make_async_copy(x_hbm.at[:, :, p], x.at[:, :, p], x_sem.at[i]) for i, p in enumerate(parts)]
    w_in = [pltpu.make_async_copy(w_hbm.at[p], w.at[p], w_sem.at[i]) for i, p in enumerate(parts)]
    for i in range(steps):
        x_in[i].start()
        w_in[i].start()
    offset = head_rows(query_ref, offset_ref, rows)
    acc = None
    for i in range(steps):
        x_in[i].wait()
        w_in[i].wait()
        part = jnp.dot(
            x[:, :, i * DEPTH : (i + 1) * DEPTH].reshape(seqs * positions, DEPTH),
            w[i * DEPTH : (i + 1) * DEPTH],
            preferred_element_type=F32,
        )
        acc = part if acc is None else acc + part
    copies = []
    for s in range(seqs):
        turned = acc[s * positions : (s + 1) * positions].T
        out[s] = turned.reshape(out.shape[1:]).astype(BF16)
        rest = out.at[s, :, pl.ds(SIDE, out.shape[2] - SIDE)]
        copies.append(pltpu.make_async_copy(rest, out_hbm.at[s], out_sem.at[s]))
        copies[-1].start()
    slots = seqs * out.shape[1]
    half = slots // 2
    me = slot()
    for r in range(slots):
        to = me ^ r
        at = ROWS + r % half * SIDE
        side_ref = send_ref if r >= half else keep_ref
        side_ref[at : at + SIDE] = out[to // out.shape[1], to % out.shape[1], :SIDE]
    state = stick(out, rows, offset, offset_ref.shape[0] // KVH)
    keep_ref[:ROWS] = state
    send_ref[:ROWS] = state
    for copy in copies:
        copy.wait()


def project(tokens, kv_weight, queries, score_offset, blocks):
    seqs, positions, depth = tokens.shape
    features = kv_weight.shape[1]
    shape = (seqs, blocks, features // blocks, positions)
    rest = (seqs, blocks, features // blocks - SIDE, positions)
    side = jax.ShapeDtypeStruct((ROWS + seqs * blocks // 2 * SIDE, LANES), BF16)
    dma = pltpu.SemaphoreType.DMA
    return pl.pallas_call(
        project_kernel,
        in_specs=[
            pl.BlockSpec(memory_space=pltpu.HBM),
            pl.BlockSpec(memory_space=pltpu.HBM),
            pl.BlockSpec(memory_space=VMEM),
            pl.BlockSpec(memory_space=pltpu.SMEM),
        ],
        out_specs=[pl.BlockSpec(memory_space=pltpu.HBM)] + [pl.BlockSpec(memory_space=VMEM)] * 2,
        out_shape=[jax.ShapeDtypeStruct(rest, BF16), side, side],
        scratch_shapes=[
            VMEM(tokens.shape, BF16),
            VMEM(kv_weight.shape, BF16),
            VMEM(shape, BF16),
            VMEM((seqs * SLOT, LANES), F32),
            dma((depth // DEPTH,)),
            dma((depth // DEPTH,)),
            dma((seqs,)),
        ],
        name="project",
    )(tokens, kv_weight, queries, score_offset)


def slot():
    return lax.axis_index("sp_0") * 8 + lax.axis_index("sp_1")


def partner(block, axis, distance):
    return lax.ppermute(block, axis, [(i, i ^ distance) for i in range(lax.axis_size(axis))])


def small(mebibytes):
    return pltpu.CompilerParams(vmem_limit_bytes=mebibytes * 1024 * 1024)


def merge(place, states):
    run = None
    for at in reversed(range(len(states))):
        state = states[0]
        for i in range(1, len(states)):
            state = choose((place ^ at) == i, states[i], state)
        run = state if run is None else fold(state, run)
    return run


def states_of(ref):
    return [unpack(ref[i * ROWS : (i + 1) * ROWS]) for i in range(2)]


def move(from_ref, source, to_ref, target, base):
    to_ref[2 * ROWS + target * SIDE : 2 * ROWS + (target + 1) * SIDE] = from_ref[
        base + source * SIDE : base + (source + 1) * SIDE
    ]


def pair_kernel(*refs):
    in_refs, out_refs = refs[:2], refs[2:]
    for low, out_ref in enumerate(out_refs):
        for i, in_ref in enumerate(in_refs):
            out_ref[i * ROWS : (i + 1) * ROWS] = in_ref[:ROWS]
            for z in range(4):
                for high in range(2):
                    move(in_ref, z * 8 + high * 4 + low, out_ref, i * 8 + z * 2 + high, ROWS)


def join_low_kernel(*refs):
    in_refs, out_refs = refs[:4], refs[4:]
    found = [states_of(ref) for ref in in_refs]
    place = lax.axis_index("sp_1") % 4
    for i in range(2):
        values, total = merge(place, [states[i] for states in found])
        state = pack(values, jnp.broadcast_to(total, (8, LANES)))
        for out_ref in out_refs:
            out_ref[i * ROWS : (i + 1) * ROWS] = state
    for high, out_ref in enumerate(out_refs):
        for low, in_ref in enumerate(in_refs):
            for i in range(2):
                for z in range(4):
                    move(in_ref, i * 8 + z * 2 + high, out_ref, low * 8 + i * 4 + z, 2 * ROWS)


def join_high_kernel(*refs):
    in_refs, out_refs = refs[:2], refs[2:]
    found = [states_of(ref) for ref in in_refs]
    place = lax.axis_index("sp_1") // 4
    for i in range(2):
        values, total = merge(place, [states[i] for states in found])
        state = pack(values, jnp.broadcast_to(total, (8, LANES)))
        for out_ref in out_refs:
            out_ref[i * ROWS : (i + 1) * ROWS] = state
    for z, out_ref in enumerate(out_refs):
        for high, in_ref in enumerate(in_refs):
            for low in range(4):
                for i in range(2):
                    move(in_ref, low * 8 + i * 4 + z, out_ref, high * 8 + low * 2 + i, 2 * ROWS)


def exchange(kernel, arrived, count):
    shape = jax.ShapeDtypeStruct((2 * ROWS + 64 // count * SIDE, LANES), BF16)
    return pl.pallas_call(
        kernel,
        in_specs=[pl.BlockSpec(memory_space=VMEM)] * len(arrived),
        out_specs=[pl.BlockSpec(memory_space=VMEM)] * count,
        out_shape=[shape] * count,
        compiler_params=small(3),
    )(*arrived)


def finish_kernel(heads, *refs):
    in_refs, (out_ref, cache_hbm, turned, wide, side, sem) = refs[:4], refs[5:]
    seqs = out_ref.shape[0]
    me = slot()
    for z, in_ref in enumerate(in_refs):
        for high in range(2):
            for low in range(4):
                for i in range(2):
                    at = 2 * ROWS + (high * 8 + low * 2 + i) * SIDE
                    source = me ^ (i * 32 + z * 8 + high * 4 + low)
                    place = pl.ds(pl.multiple_of(source * LANES, LANES), LANES)
                    side[:, place] = in_ref[at : at + SIDE]
    copy = pltpu.make_async_copy(side, cache_hbm.at[pl.ds(0, SIDE)], sem)
    copy.start()
    found = [states_of(ref) for ref in in_refs]
    values, _ = merge(lax.axis_index("sp_0"), [states[i] for i in range(2) for states in found])
    turned[...] = jnp.concatenate([values, values], axis=0).T
    for h in range(heads):
        wide[:, h * HD : (h + 1) * HD] = turned[pl.ds(h, seqs, stride=SLOT), :][:, :HD]
    out_ref[...] = wide[...].astype(out_ref.dtype)
    copy.wait()


def finish(arrived, laid, seqs, heads):
    return pl.pallas_call(
        functools.partial(finish_kernel, heads),
        in_specs=[pl.BlockSpec(memory_space=VMEM)] * len(arrived)
        + [pl.BlockSpec(memory_space=pl.ANY)],
        out_specs=[pl.BlockSpec(memory_space=VMEM), pl.BlockSpec(memory_space=pl.ANY)],
        out_shape=[
            jax.ShapeDtypeStruct((seqs, heads * HD), BF16),
            jax.ShapeDtypeStruct(laid.shape, BF16),
        ],
        scratch_shapes=[
            VMEM((LANES, LANES), F32),
            VMEM((seqs, heads * HD), F32),
            VMEM((SIDE, laid.shape[1]), BF16),
            pltpu.SemaphoreType.DMA,
        ],
        input_output_aliases={len(arrived): 1},
        compiler_params=small(3),
        name="finish",
    )(*arrived, laid)


def lay_kernel(in_ref, out_ref, sem):
    sources, width, positions = in_ref.shape
    rest = pl.ds(SIDE, width)
    for i in range(sources):
        place = pl.ds(i * positions, positions)
        pltpu.make_async_copy(in_ref.at[i], out_ref.at[rest, place], sem).start()
    pltpu.make_async_copy(out_ref.at[rest], out_ref.at[rest], sem).wait()


def lay(received):
    sources, width, positions = received.shape
    return pl.pallas_call(
        lay_kernel,
        in_specs=[pl.BlockSpec(memory_space=pl.ANY)],
        out_specs=pl.BlockSpec(memory_space=pl.ANY),
        out_shape=jax.ShapeDtypeStruct((SIDE + width, sources * positions), received.dtype),
        scratch_shapes=[pltpu.SemaphoreType.DMA],
        compiler_params=small(1),
        name="lay",
    )(received)


def local(tokens, kv_weight, queries, score_offset):
    seqs, positions, _ = tokens.shape
    features = kv_weight.shape[1]
    slots = lax.axis_size(SP)
    blocks = slots // seqs
    width = features // blocks
    heads = score_offset.shape[0]

    projected, keep, send = project(tokens, kv_weight, queries, score_offset, blocks)
    opposite = partner(send, "sp_0", 4)
    received = lax.all_to_all(
        projected.reshape(slots, width - SIDE, positions),
        SP,
        split_axis=0,
        concat_axis=0,
        tiled=True,
    )
    laid = lay(received)
    parts = exchange(pair_kernel, [keep, opposite], 4)
    parts = [parts[0]] + [partner(parts[d], "sp_1", d) for d in (1, 2, 3)]
    parts = exchange(join_low_kernel, parts, 2)
    parts = [parts[0]] + [partner(parts[1], "sp_1", 4)]
    parts = exchange(join_high_kernel, parts, 4)
    arrived = [parts[0]]
    for distance in (1, 2, 3):
        arrived.append(partner(parts[distance], "sp_0", distance))
    read, cache = finish(arrived, laid, seqs, heads)
    return cache.T.reshape(1, 1, slots * positions, width), read


def solution(mesh):
    torus = Mesh(
        mesh.devices.reshape(mesh.shape["gr"], 8, 8, mesh.shape["tp"]), ("gr", "sp_0", "sp_1", "tp")
    )
    return jax.shard_map(
        local,
        mesh=torus,
        in_specs=(P(("gr", "tp"), SP, None), P(), P(("gr", "tp"), None), P()),
        out_specs=(P(("gr", "tp"), SP, None, None), P(("gr", "tp"), None)),
        check_vma=False,
    )
```

```python
import functools

import jax
import jax.numpy as jnp
from jax import lax
from jax.experimental import pallas as pl
from jax.experimental.pallas import tpu as pltpu
from jax.sharding import Mesh
from jax.sharding import PartitionSpec as P


KVH = 8
HD = 64
LANES = 128
SLOT = 32
SIDE = 8
ROWS = HD + 8
DEPTH = 256
SP = ("sp_0", "sp_1")
VMEM = pltpu.VMEM
BF16 = jnp.bfloat16
F32 = jnp.float32
BY_POSITION = (((1,), (1,)), ((), ()))


def pack(values, total):
    high = total.astype(BF16).astype(F32)
    middle = (total - high).astype(BF16).astype(F32)
    row = lax.broadcasted_iota(jnp.int32, total.shape, 0)
    parts = jnp.where(row == 0, high, jnp.where(row == 1, middle, total - high - middle))
    return jnp.concatenate([values, parts], axis=0).astype(BF16)


def unpack(state):
    state = state.astype(F32)
    return state[:HD], state[HD : HD + 1] + state[HD + 1 : HD + 2] + state[HD + 2 : HD + 3]


def fold(first, last):
    return first[0] * jnp.exp(last[1]) + last[0], first[1] + last[1]


def choose(condition, one, other):
    return tuple(jnp.where(condition, a, b) for a, b in zip(one, other))


def head_rows(query_ref, offset_ref, rows):
    seqs = query_ref.shape[0]
    heads = offset_ref.shape[0]
    rows[...] = jnp.zeros_like(rows)
    row = lax.broadcasted_iota(jnp.int32, (SLOT, LANES), 0)
    offset = jnp.zeros((SLOT, LANES), F32)
    for h in range(heads):
        query = query_ref[:, h * HD : (h + 1) * HD].astype(F32)
        rows[pl.ds(h, seqs, stride=SLOT), :] = jnp.concatenate([query, query], axis=1)
        offset = jnp.where(row == h, offset_ref[h], offset)
    return offset


def split(x, parts):
    pieces = []
    for _ in range(parts):
        piece = x.astype(BF16)
        pieces.append(piece)
        x = x - piece.astype(F32)
    return jnp.concatenate(pieces, axis=0)


def stick(kv, rows, offset, group):
    seqs = kv.shape[0]
    slots = seqs * SLOT
    row_head = lax.broadcasted_iota(jnp.int32, (SLOT, LANES), 0) // group
    odd = lax.broadcasted_iota(jnp.int32, (SLOT, LANES), 1) // HD
    logits = []
    for s in range(seqs):
        queries = rows[s * SLOT : (s + 1) * SLOT]
        own = [jnp.where(row_head == n + odd, queries, 0.0) for n in range(0, KVH, 2)]
        keys = kv[s, :KVH].reshape(KVH * HD, LANES)
        total = jnp.dot(
            jnp.concatenate(own, axis=1).astype(BF16), keys, preferred_element_type=F32
        )
        logits.append(total * HD ** (-0.5) + offset)
    logit = jnp.concatenate(logits, axis=0)
    soft = jnp.log1p(jnp.exp(-jnp.abs(logit)))
    log_take = jnp.minimum(logit, 0.0) - soft
    keep = jnp.minimum(-logit, 0.0) - soft
    r = lax.broadcasted_iota(jnp.int32, (LANES, LANES), 0)
    c = lax.broadcasted_iota(jnp.int32, (LANES, LANES), 1)
    sums = jnp.dot(split(keep, 3), (r > c).astype(BF16), preferred_element_type=F32)
    between = sums[:slots] + sums[slots : 2 * slots] + sums[2 * slots :]
    weight = jnp.exp(log_take + between)
    read = []
    for s in range(seqs):
        weights = split(weight[s * SLOT : (s + 1) * SLOT], 2)
        values = kv[s, KVH:].reshape(KVH * HD, LANES)
        product = lax.dot_general(weights, values, BY_POSITION, preferred_element_type=F32)
        product = product[:SLOT] + product[SLOT:]
        halves = [jnp.zeros((SLOT, LANES), F32), jnp.zeros((SLOT, LANES), F32)]
        for n in range(KVH):
            piece = product[:, n // 2 * LANES : (n // 2 + 1) * LANES]
            halves[n % 2] = jnp.where(row_head == n, piece, halves[n % 2])
        read.append(jnp.where(row_head % 2 == 0, halves[0], pltpu.roll(halves[1], HD, 1)))
    total = (between + keep)[:, :1]
    state = jnp.where(c < HD, jnp.concatenate(read, axis=0), total).T
    return pack(state[:HD], state[HD:ROWS])


def project_kernel(
    x_hbm,
    w_hbm,
    query_ref,
    offset_ref,
    out_hbm,
    keep_ref,
    send_ref,
    x,
    w,
    out,
    rows,
    x_sem,
    w_sem,
    out_sem,
):
    seqs, positions, depth = x.shape
    steps = depth // DEPTH
    parts = [pl.ds(i * DEPTH, DEPTH) for i in range(steps)]
    x_in = [pltpu.make_async_copy(x_hbm.at[:, :, p], x.at[:, :, p], x_sem.at[i]) for i, p in enumerate(parts)]
    w_in = [pltpu.make_async_copy(w_hbm.at[p], w.at[p], w_sem.at[i]) for i, p in enumerate(parts)]
    for i in range(steps):
        x_in[i].start()
        w_in[i].start()
    offset = head_rows(query_ref, offset_ref, rows)
    acc = None
    for i in range(steps):
        x_in[i].wait()
        w_in[i].wait()
        part = jnp.dot(
            x[:, :, i * DEPTH : (i + 1) * DEPTH].reshape(seqs * positions, DEPTH),
            w[i * DEPTH : (i + 1) * DEPTH],
            preferred_element_type=F32,
        )
        acc = part if acc is None else acc + part
    copies = []
    for s in range(seqs):
        turned = acc[s * positions : (s + 1) * positions].T
        out[s] = turned.reshape(out.shape[1:]).astype(BF16)
        rest = out.at[s, :, pl.ds(SIDE, out.shape[2] - SIDE)]
        copies.append(pltpu.make_async_copy(rest, out_hbm.at[s], out_sem.at[s]))
        copies[-1].start()
    slots = seqs * out.shape[1]
    half = slots // 2
    me = slot()
    for r in range(slots):
        to = me ^ r
        at = ROWS + r % half * SIDE
        side_ref = send_ref if r >= half else keep_ref
        side_ref[at : at + SIDE] = out[to // out.shape[1], to % out.shape[1], :SIDE]
    state = stick(out, rows, offset, offset_ref.shape[0] // KVH)
    keep_ref[:ROWS] = state
    send_ref[:ROWS] = state
    for copy in copies:
        copy.wait()


def project(tokens, kv_weight, queries, score_offset, blocks):
    seqs, positions, depth = tokens.shape
    features = kv_weight.shape[1]
    shape = (seqs, blocks, features // blocks, positions)
    rest = (seqs, blocks, features // blocks - SIDE, positions)
    side = jax.ShapeDtypeStruct((ROWS + seqs * blocks // 2 * SIDE, LANES), BF16)
    dma = pltpu.SemaphoreType.DMA
    return pl.pallas_call(
        project_kernel,
        in_specs=[
            pl.BlockSpec(memory_space=pltpu.HBM),
            pl.BlockSpec(memory_space=pltpu.HBM),
            pl.BlockSpec(memory_space=VMEM),
            pl.BlockSpec(memory_space=pltpu.SMEM),
        ],
        out_specs=[pl.BlockSpec(memory_space=pltpu.HBM)] + [pl.BlockSpec(memory_space=VMEM)] * 2,
        out_shape=[jax.ShapeDtypeStruct(rest, BF16), side, side],
        scratch_shapes=[
            VMEM(tokens.shape, BF16),
            VMEM(kv_weight.shape, BF16),
            VMEM(shape, BF16),
            VMEM((seqs * SLOT, LANES), F32),
            dma((depth // DEPTH,)),
            dma((depth // DEPTH,)),
            dma((seqs,)),
        ],
        name="project",
    )(tokens, kv_weight, queries, score_offset)


def slot():
    return lax.axis_index("sp_0") * 8 + lax.axis_index("sp_1")


def partner(block, axis, distance):
    return lax.ppermute(block, axis, [(i, i ^ distance) for i in range(lax.axis_size(axis))])


def small(mebibytes):
    return pltpu.CompilerParams(vmem_limit_bytes=mebibytes * 1024 * 1024)


def merge(place, states):
    run = None
    for at in reversed(range(len(states))):
        state = states[0]
        for i in range(1, len(states)):
            state = choose((place ^ at) == i, states[i], state)
        run = state if run is None else fold(state, run)
    return run


def states_of(ref):
    return [unpack(ref[i * ROWS : (i + 1) * ROWS]) for i in range(2)]


def move(from_ref, source, to_ref, target, base):
    to_ref[2 * ROWS + target * SIDE : 2 * ROWS + (target + 1) * SIDE] = from_ref[
        base + source * SIDE : base + (source + 1) * SIDE
    ]


def pair_kernel(*refs):
    in_refs, out_refs = refs[:2], refs[2:]
    for low, out_ref in enumerate(out_refs):
        for i, in_ref in enumerate(in_refs):
            out_ref[i * ROWS : (i + 1) * ROWS] = in_ref[:ROWS]
            for z in range(4):
                for high in range(2):
                    move(in_ref, z * 8 + high * 4 + low, out_ref, i * 8 + z * 2 + high, ROWS)


def join_low_kernel(*refs):
    in_refs, out_refs = refs[:4], refs[4:]
    found = [states_of(ref) for ref in in_refs]
    place = lax.axis_index("sp_1") % 4
    for i in range(2):
        values, total = merge(place, [states[i] for states in found])
        state = pack(values, jnp.broadcast_to(total, (8, LANES)))
        for out_ref in out_refs:
            out_ref[i * ROWS : (i + 1) * ROWS] = state
    for high, out_ref in enumerate(out_refs):
        for low, in_ref in enumerate(in_refs):
            for i in range(2):
                for z in range(4):
                    move(in_ref, i * 8 + z * 2 + high, out_ref, low * 8 + i * 4 + z, 2 * ROWS)


def join_high_kernel(*refs):
    in_refs, out_refs = refs[:2], refs[2:]
    found = [states_of(ref) for ref in in_refs]
    place = lax.axis_index("sp_1") // 4
    for i in range(2):
        values, total = merge(place, [states[i] for states in found])
        state = pack(values, jnp.broadcast_to(total, (8, LANES)))
        for out_ref in out_refs:
            out_ref[i * ROWS : (i + 1) * ROWS] = state
    for z, out_ref in enumerate(out_refs):
        for high, in_ref in enumerate(in_refs):
            for low in range(4):
                for i in range(2):
                    move(in_ref, low * 8 + i * 4 + z, out_ref, high * 8 + low * 2 + i, 2 * ROWS)


def exchange(kernel, arrived, count):
    shape = jax.ShapeDtypeStruct((2 * ROWS + 64 // count * SIDE, LANES), BF16)
    return pl.pallas_call(
        kernel,
        in_specs=[pl.BlockSpec(memory_space=VMEM)] * len(arrived),
        out_specs=[pl.BlockSpec(memory_space=VMEM)] * count,
        out_shape=[shape] * count,
        compiler_params=small(3),
    )(*arrived)


def finish_kernel(heads, *refs):
    in_refs, (out_ref, cache_hbm, turned, wide, side, sem) = refs[:4], refs[5:]
    seqs = out_ref.shape[0]
    me = slot()
    for z, in_ref in enumerate(in_refs):
        for high in range(2):
            for low in range(4):
                for i in range(2):
                    at = 2 * ROWS + (high * 8 + low * 2 + i) * SIDE
                    source = me ^ (i * 32 + z * 8 + high * 4 + low)
                    place = pl.ds(pl.multiple_of(source * LANES, LANES), LANES)
                    side[:, place] = in_ref[at : at + SIDE]
    copy = pltpu.make_async_copy(side, cache_hbm.at[pl.ds(0, SIDE)], sem)
    copy.start()
    found = [states_of(ref) for ref in in_refs]
    values, _ = merge(lax.axis_index("sp_0"), [states[i] for i in range(2) for states in found])
    turned[...] = jnp.concatenate([values, values], axis=0).T
    for h in range(heads):
        wide[:, h * HD : (h + 1) * HD] = turned[pl.ds(h, seqs, stride=SLOT), :][:, :HD]
    out_ref[...] = wide[...].astype(out_ref.dtype)
    copy.wait()


def finish(arrived, laid, seqs, heads):
    return pl.pallas_call(
        functools.partial(finish_kernel, heads),
        in_specs=[pl.BlockSpec(memory_space=VMEM)] * len(arrived)
        + [pl.BlockSpec(memory_space=pl.ANY)],
        out_specs=[pl.BlockSpec(memory_space=VMEM), pl.BlockSpec(memory_space=pl.ANY)],
        out_shape=[
            jax.ShapeDtypeStruct((seqs, heads * HD), BF16),
            jax.ShapeDtypeStruct(laid.shape, BF16),
        ],
        scratch_shapes=[
            VMEM((LANES, LANES), F32),
            VMEM((seqs, heads * HD), F32),
            VMEM((SIDE, laid.shape[1]), BF16),
            pltpu.SemaphoreType.DMA,
        ],
        input_output_aliases={len(arrived): 1},
        compiler_params=small(3),
        name="finish",
    )(*arrived, laid)


def lay_kernel(in_ref, out_ref, sem):
    sources, width, positions = in_ref.shape
    rest = pl.ds(SIDE, width)
    for i in range(sources):
        place = pl.ds(i * positions, positions)
        pltpu.make_async_copy(in_ref.at[i], out_ref.at[rest, place], sem).start()
    pltpu.make_async_copy(out_ref.at[rest], out_ref.at[rest], sem).wait()


def lay(received):
    sources, width, positions = received.shape
    return pl.pallas_call(
        lay_kernel,
        in_specs=[pl.BlockSpec(memory_space=pl.ANY)],
        out_specs=pl.BlockSpec(memory_space=pl.ANY),
        out_shape=jax.ShapeDtypeStruct((SIDE + width, sources * positions), received.dtype),
        scratch_shapes=[pltpu.SemaphoreType.DMA],
        compiler_params=small(1),
        name="lay",
    )(received)


def local(tokens, kv_weight, queries, score_offset):
    seqs, positions, _ = tokens.shape
    features = kv_weight.shape[1]
    slots = lax.axis_size(SP)
    blocks = slots // seqs
    width = features // blocks
    heads = score_offset.shape[0]

    projected, keep, send = project(tokens, kv_weight, queries, score_offset, blocks)
    opposite = partner(send, "sp_0", 4)
    received = lax.all_to_all(
        projected.reshape(slots, width - SIDE, positions),
        SP,
        split_axis=0,
        concat_axis=0,
        tiled=True,
    )
    laid = lay(received)
    parts = exchange(pair_kernel, [keep, opposite], 4)
    parts = [parts[0]] + [partner(parts[d], "sp_1", d) for d in (1, 2, 3)]
    parts = exchange(join_low_kernel, parts, 2)
    parts = [parts[0]] + [partner(parts[1], "sp_1", 4)]
    parts = exchange(join_high_kernel, parts, 4)
    arrived = [parts[0]]
    for distance in (1, 2, 3):
        arrived.append(partner(parts[distance], "sp_0", distance))
    read, cache = finish(arrived, laid, seqs, heads)
    return cache.T.reshape(1, 1, slots * positions, width), read


def solution(mesh):
    torus = Mesh(
        mesh.devices.reshape(mesh.shape["gr"], 8, 8, mesh.shape["tp"]), ("gr", "sp_0", "sp_1", "tp")
    )
    return jax.shard_map(
        local,
        mesh=torus,
        in_specs=(P(("gr", "tp"), SP, None), P(), P(("gr", "tp"), None), P()),
        out_specs=(P(("gr", "tp"), SP, None, None), P(("gr", "tp"), None)),
        check_vma=False,
    )
```
